32 devices in a mesh: ep: 8 (over z, core), tp: 4 (over y, x).
Axes of the slice: x: 2, y: 2, z: 4, core: 2. Of those that a mesh axis runs over, the one named last changes fastest.
Arguments:
- tokens: bfloat16 [256, 2048], P('ep', 'tp'), may hold values from -200 to 200
- routing: int32 [256, 4], P('ep'), may hold values from 0 to 15, all different within a row; in each aligned block of 32 rows (0 to 31, 32 to 63, ...) at most 8 rows name the same one
- gate_weights: float32 [256, 4], P('ep'), may hold values from 0.05 to 1
- norm_gain: float32 [2048], replicated, may hold values from 0.1 to 1.9
- w_gate: bfloat16 [16, 2048, 2048], P('ep', None, 'tp'), may hold values from -0.33007812 to 0.33007812
- w_up: bfloat16 [16, 2048, 2048], P('ep', None, 'tp'), may hold values from -0.33007812 to 0.33007812
- w_down: bfloat16 [16, 2048, 2048], P('ep', 'tp'), may hold values from -0.026489258 to 0.026489258
Outputs:
- mixed: bfloat16 [256, 2048], P('ep', 'tp')
The draws below stay inside these ranges and needn't reach their ends.
Inputs may be any that keep to these rules, and one draw needn't show every extreme that they name: `routing`: each token names 4 different experts. Among the 32 tokens of one index of ep no expert is named more than 8 times, a bound that some block reaches.
All inputs are finite; a program needn't handle non-finite values.
Results may differ from the reference program's by a relative error of at most 0.015.
Values may be sent and summed in bfloat16 or wider, within the bound.
A program may use at most 128 MiB of HBM per device.

```python
import math
import jax
import jax.numpy as jnp
import numpy as np
from jax import lax

D = 2048
FF = 2048
TOP = 4
EXP_DEV = 2
TOK_DEV = 32
CAP = 8
EXPERTS = 16
TOKENS = 256
N_EP = 8
N_TP = 4


def draw_tokens(key, part):
    base_key, scale_key, row_key, mean_key = jax.random.split(key, 4)
    values = jax.random.normal(base_key, (TOKENS, D), jnp.float32)
    values = jnp.clip(values, -6.0, 6.0)
    column_scale = jnp.exp(jax.random.uniform(scale_key, (D // 16,), jnp.float32, jnp.log(0.3), jnp.log(3.0)))
    values = values * jnp.repeat(column_scale, 16)[None, :]
    return values.astype(jnp.bfloat16)


def block_levels(stream_key, dims, cuts, smallest, top_value):
    loudness = 1.0
    for axis_at, shards_of in cuts:
        draws = jax.random.uniform(jax.random.fold_in(jax.random.fold_in(stream_key, 6), axis_at), (shards_of,), jnp.float32, smallest / len(cuts), top_value / len(cuts))
        loudness = loudness * jnp.repeat(jnp.exp(draws), dims[axis_at] // shards_of).reshape((-1,) + (1,) * (len(dims) - 1 - axis_at))
    return loudness


def routed_block(key, own, number, rows, count, top, most, skew):
    order = jax.random.permutation(key, count)
    crowded, common = load_shares(count, rows * top, most, skew, True), load_shares(count, rows * top, most, skew, False)
    places = jnp.arange(count)

    def named(lengths, rotation):
        used = int((lengths > 0).sum())
        fixed = max(1, used // 4)
        moved = fixed + (places - fixed + rotation * (used - fixed)) % max(1, count - fixed)
        return jnp.zeros((count,), jnp.int32).at[order[jnp.where(places < fixed, places, moved)]].set(jnp.asarray(lengths, jnp.int32))

    lengths = jnp.where(number % 4 == 0, named(crowded, number // 4), named(common, number - number // 4 - 1))
    mixed = jax.random.permutation(jax.random.fold_in(own, 3), count)
    giver, taker = mixed[0:count // 2 * 2:2], mixed[1:count // 2 * 2:2]
    room = jnp.minimum(lengths[giver] - 1, most - lengths[taker]) // 2
    room = jnp.where((giver == order[0]) | (taker == order[0]) | (lengths[taker] == 0), 0, jnp.maximum(room, 0))
    moved = jax.random.randint(jax.random.fold_in(own, 4), (count // 2,), 0, 1 << 20) % (room + 1)
    lengths = lengths.at[giver].add(-moved).at[taker].add(moved)
    members = jnp.searchsorted(jnp.cumsum(lengths), jnp.arange(rows * top), side="right").astype(jnp.int32)
    listing = members.reshape(top, rows).T
    listing = listing[jax.random.permutation(jax.random.fold_in(own, 1), rows)]
    rotation = jax.random.randint(jax.random.fold_in(own, 2), (rows, 1), 0, top)
    return jnp.take_along_axis(listing, (jnp.arange(top)[None, :] + rotation) % top, axis=1)


def load_shares(amount, total, most, slope, full):
    weights = [(1 << 20) // math.isqrt(grade ** slope) + 1 for grade in range(1, amount + 1)]
    largest = most if full else min(most, max(-(-total // amount), total * weights[0] // sum(weights)))
    least = 1 if total - largest >= amount - 1 else 0
    counts, rest = [largest] + [least] * (amount - 1), total - largest - least * (amount - 1)
    while rest > 0:
        free = [i for i in range(1, amount) if counts[i] < largest] or [i for i in range(1, amount) if counts[i] < most]
        whole, left = sum([weights[i] for i in free]), rest
        for i in free:
            more = min(most - counts[i], max(1, left * weights[i] // whole), rest)
            counts[i] = counts[i] + more
            rest = rest - more
    return np.array(counts)


def scatter_about(key, shape, deviation, reach, pieces=(), held_as=jnp.bfloat16):
    drawn = deviation * jax.random.normal(key, shape, jnp.float32)
    if pieces:
        drawn = drawn * block_levels(key, shape, pieces, -0.22, 0.18)
    return jnp.clip(drawn, -reach, reach).astype(held_as)


def setup_inputs(seed: int = 0) -> dict:
    keys = jax.random.split(jax.random.key(seed), 8)
    tokens = draw_tokens(jax.random.fold_in(keys[7], 71), 0)
    routing_keys = jax.random.split(jax.random.fold_in(keys[1], 1), TOKENS // TOK_DEV)
    routing_turns = jax.random.permutation(jax.random.fold_in(keys[1], 3), TOKENS // TOK_DEV)
    routing = jax.vmap(lambda own, number: routed_block(jax.random.fold_in(keys[1], 2), own, number, TOK_DEV, EXP_DEV * N_EP, TOP, CAP, 2))(routing_keys, routing_turns).reshape((TOKENS, TOP))
    gate_weights = jnp.clip(jnp.exp(math.log(1.0) - 2.9957323 * jax.random.uniform(keys[2], (TOKENS, TOP), jnp.float32) ** block_levels(keys[2], (TOKENS, TOP), ((0, 8),), -0.2, 0.2)), 0.05, 1.0)
    norm_gain = jnp.clip(1.0 + 0.18 * jax.random.normal(keys[3], (D,), jnp.float32), 0.1, 1.9)
    w_gate = scatter_about(keys[4], (EXPERTS, D, FF), (2.5 * D ** -0.5), 0.33007812, ((0, 8), (2, 4)))
    w_up = scatter_about(keys[5], (EXPERTS, D, FF), (2.5 * D ** -0.5), 0.33007812, ((0, 8), (2, 4)))
    w_down = scatter_about(keys[6], (EXPERTS, FF, D), (0.2 * FF ** -0.5), 0.026489258, ((0, 8), (1, 4)))
    return dict(tokens=tokens, routing=routing, gate_weights=gate_weights, norm_gain=norm_gain, w_gate=w_gate, w_up=w_up, w_down=w_down)


norm_eps = 1e-06
clamp_limit = 7.0
swish_alpha = 1.702

def expert_apply(inputs):
    rows, gate_mat, up_mat, down_mat = inputs
    pre_gate = jnp.dot(rows, gate_mat, preferred_element_type=jnp.float32)
    pre_up = jnp.dot(rows, up_mat, preferred_element_type=jnp.float32)
    clamped = jnp.minimum(pre_gate, clamp_limit)
    upper = jnp.clip(pre_up, -clamp_limit, clamp_limit)
    hidden = (clamped * jax.nn.sigmoid(swish_alpha * clamped) * (upper + 1.0)).astype(jnp.bfloat16)
    block_width = FF // N_TP
    hidden_blocks = hidden.reshape(hidden.shape[0], N_TP, block_width).astype(jnp.float32)
    down_blocks = down_mat.reshape(N_TP, block_width, D).astype(jnp.float32)
    partial_value = jnp.einsum('rnf,nfd->nrd', hidden_blocks, down_blocks)
    rounded = partial_value.astype(jnp.bfloat16).astype(jnp.float32)
    return lax.optimization_barrier(jnp.sum(rounded, axis=0)).astype(jnp.bfloat16)

def reference(tokens, routing, gate_weights, norm_gain, w_gate, w_up, w_down):
    expert_count = EXP_DEV * N_EP
    wide = tokens.astype(jnp.float32)
    ssq = lax.optimization_barrier(jnp.sum(wide * wide, axis=1, keepdims=True))
    normed = (wide * lax.rsqrt(ssq / D + norm_eps) * norm_gain[None, :]).astype(jnp.bfloat16)
    grouped = routing.reshape(N_EP, TOK_DEV * TOP)
    onehot = (grouped[:, :, None] == jnp.arange(expert_count, dtype=jnp.int32)[None, None, :]).astype(jnp.int32)
    slot_rank = lax.optimization_barrier(jnp.sum(jnp.cumsum(onehot, axis=1) * onehot, axis=2)) - 1
    groups = jnp.arange(N_EP, dtype=jnp.int32)[:, None]
    slot_index = (grouped * (N_EP * CAP) + groups * CAP + slot_rank).reshape(-1).astype(jnp.int32)
    repeated = jnp.repeat(normed, TOP, axis=0)
    buffer = jnp.zeros((expert_count * N_EP * CAP, D), jnp.bfloat16).at[slot_index].set(repeated)
    buffer = buffer.reshape(expert_count, N_EP * CAP, D)
    expert_out = lax.map(expert_apply, (buffer, w_gate, w_up, w_down))
    picked = expert_out.reshape(-1, D)[slot_index].astype(jnp.float32).reshape(TOKENS, TOP, D)
    mixed = lax.optimization_barrier(jnp.sum(gate_weights[:, :, None] * picked, axis=1))
    return mixed.astype(jnp.bfloat16)
```

```python
import functools

import jax
import jax.numpy as jnp
from jax import lax
from jax.experimental import pallas as pl
from jax.experimental.pallas import tpu as pltpu
from jax.sharding import PartitionSpec as P

CAP = 8
MESH = pl.DeviceIdType.MESH

norm_eps = 1e-06
clamp_limit = 7.0
swish_alpha = 1.702


def partner(me, step, n):
    if n & (n - 1):
        return lax.rem(me + step, n)
    other, bit = 0, 1
    while bit < n:
        mine = (me // bit) % 2
        other = other + bit * ((1 - mine) if step & bit else mine)
        bit *= 2
    return other


def nearest(me, step, n):
    bound = n * n
    found = 0
    for at in range(n):
        by_distance = sorted(range(n), key=lambda other: (abs(other - at), other))
        apart = (me - at) * (me - at)
        found = found + by_distance[step] * (1 - lax.div(apart + (bound - 1), bound))
    return found


def kernel(
    n_ep,
    n_tp,
    tok_hbm,
    rout_hbm,
    gw_hbm,
    gain_hbm,
    wg_hbm,
    wu_hbm,
    wd_hbm,
    out_ref,
    tok_ref,
    rout_ref,
    gw_ref,
    gain_ref,
    wg,
    wu,
    wd,
    outgoing,
    rows,
    combine,
    acc_gate,
    acc_up,
    part,
    part_in,
    ret_out,
    ret_in,
    in_sem,
    w_sem,
    disp_send,
    disp_recv,
    gath_send,
    gath_recv,
    part_send,
    part_recv,
    ret_send,
    ret_recv,
):
    ep, tp = lax.axis_index("ep"), lax.axis_index("tp")
    n_exp, width, ff = wg_hbm.shape
    n_tok, cols = tok_ref.shape
    top = rout_ref.shape[0]
    slots = n_ep * n_exp * CAP
    pair = 2 if n_ep % 2 == 0 else 1
    n_chip = n_ep // pair
    chip, core = lax.div(ep, pair), lax.rem(ep, pair)
    chips = [chip] + [nearest(chip, step, n_chip) for step in range(1, n_chip)]
    cores = [lax.rem(core + turn, pair) for turn in range(pair)]
    peers = [chips[0] * pair + k for k in cores[1:]]
    peers += [other * pair + k for other in chips[1:] for k in cores]
    hops = list(range(1, n_tp))

    small = [
        pltpu.make_async_copy(src, dst, in_sem.at[i])
        for i, (src, dst) in enumerate(
            ((rout_hbm, rout_ref), (gw_hbm, gw_ref), (tok_hbm, tok_ref), (gain_hbm, gain_ref))
        )
    ]
    for copy in small:
        copy.start()

    barrier = pltpu.get_barrier_semaphore()
    for peer in peers[::-1]:
        pl.semaphore_signal(barrier, inc=1, device_id=(peer, tp), device_id_type=MESH)
    for hop in hops[::-1]:
        pl.semaphore_signal(
            barrier, inc=1, device_id=(ep, partner(tp, hop, n_tp)), device_id_type=MESH
        )

    loads = []
    for e in range(n_exp):
        for i, (src, dst) in enumerate(((wg_hbm, wg), (wu_hbm, wu), (wd_hbm, wd))):
            loads.append(pltpu.make_async_copy(src.at[e], dst.at[e], w_sem.at[i, e]))
    for load in loads:
        load.start()

    slot = lax.broadcasted_iota(jnp.int32, (slots, n_tok), 0)
    slot_exp, slot_rank = slot // CAP, slot % CAP
    named = jnp.zeros((slots, n_tok), jnp.float32)
    weight = jnp.zeros((slots, n_tok), jnp.float32)
    small[0].wait()
    small[1].wait()
    for k in range(top):
        hit = rout_ref[k : k + 1, :] == slot_exp
        named = named + jnp.where(hit, 1.0, 0.0)
        weight = weight + jnp.where(hit, gw_ref[k : k + 1, :], 0.0)
    earlier = jnp.where(
        lax.broadcasted_iota(jnp.int32, (n_tok, n_tok), 0)
        < lax.broadcasted_iota(jnp.int32, (n_tok, n_tok), 1),
        1.0,
        0.0,
    ).astype(jnp.bfloat16)
    rank = jnp.dot(named.astype(jnp.bfloat16), earlier, preferred_element_type=jnp.float32)
    placing = jnp.where(rank == slot_rank.astype(jnp.float32), named, 0.0)
    small[2].wait()
    sent = jnp.dot(
        placing.astype(jnp.bfloat16), tok_ref[...], preferred_element_type=jnp.float32
    )
    outgoing[...] = sent.astype(jnp.bfloat16).reshape(n_ep, n_exp, CAP, cols)
    rows[tp, ep] = outgoing[ep]

    pl.semaphore_wait(barrier, n_ep - 1 + n_tp - 1)

    def dispatch(peer):
        return pltpu.make_async_remote_copy(
            src_ref=outgoing.at[peer],
            dst_ref=rows.at[tp, ep],
            send_sem=disp_send,
            recv_sem=disp_recv.at[chip],
            device_id=(peer, tp),
            device_id_type=MESH,
        )

    def gather(src, hop, s, count, c):
        return pltpu.make_async_remote_copy(
            src_ref=src,
            dst_ref=rows.at[tp, pl.ds(s, count)],
            send_sem=gath_send,
            recv_sem=gath_recv.at[tp, c],
            device_id=(ep, partner(tp, hop, n_tp)),
            device_id_type=MESH,
        )

    def reduce(hop, e, c):
        q = partner(tp, hop, n_tp)
        return pltpu.make_async_remote_copy(
            src_ref=part.at[q, pl.ds(c * pair, pair), e],
            dst_ref=part_in.at[e, c, hop - 1],
            send_sem=part_send,
            recv_sem=part_recv.at[e, c],
            device_id=(ep, q),
            device_id_type=MESH,
        )

    def give_back(peer, e):
        return pltpu.make_async_remote_copy(
            src_ref=ret_out.at[peer, e],
            dst_ref=ret_in.at[ep, e],
            send_sem=ret_send,
            recv_sem=ret_recv,
            device_id=(peer, tp),
            device_id_type=MESH,
        )

    def landed(ref, sem):
        pltpu.make_async_copy(ref, ref, sem).wait()

    def finish(pre_gate, pre_up, factor, e):
        clamped = jnp.minimum(pre_gate * factor, clamp_limit)
        upper = jnp.clip(pre_up * factor, -clamp_limit, clamp_limit)
        hidden = (clamped * jax.nn.sigmoid(swish_alpha * clamped) * (upper + 1.0)).astype(
            jnp.bfloat16
        )
        loads[3 * e + 2].wait()
        for hop in hops[::-1] + [0]:
            q = partner(tp, hop, n_tp) if hop else tp
            at = pl.multiple_of(q * cols, cols)
            part[q, :, e] = (
                jnp.dot(hidden, wd[e, :, pl.ds(at, cols)], preferred_element_type=jnp.float32)
                .reshape(n_ep, CAP, cols)
                .astype(jnp.bfloat16)
            )
            if hop:
                for c in chips[::-1]:
                    reduce(hop, e, c).start()

    for peer in peers[::-1]:
        dispatch(peer).start()
    for hop in hops[::-1]:
        gather(outgoing.at[pl.ds(ep, 1)], hop, ep, 1, chip).start()

    def take(j, e):
        wide = rows[j, :, e].astype(jnp.float32)
        at = pl.multiple_of(j * cols, cols)
        x = wide * gain_ref[:, pl.ds(at, cols)].reshape(1, 1, cols)
        x = x.reshape(n_ep * CAP, cols).astype(jnp.bfloat16)
        y = [
            jnp.dot(x, w[e, pl.ds(at, cols), :], preferred_element_type=jnp.float32)
            for w in (wg, wu)
        ]
        return y, jnp.sum(wide * wide, axis=2, keepdims=True)

    for c in chips:
        if c is chips[0]:
            for s in peers[: pair - 1]:
                landed(rows.at[tp, s], disp_recv.at[c])
                for hop in hops[::-1]:
                    gather(rows.at[tp, pl.ds(s, 1)], hop, s, 1, c).start()
        else:
            here = rows.at[tp, pl.ds(c * pair, pair)]
            landed(here, disp_recv.at[c])
            for hop in hops[::-1]:
                gather(here, hop, c * pair, pair, c).start()
    small[3].wait()
    squares = []
    for e in range(n_exp):
        loads[3 * e].wait()
        loads[3 * e + 1].wait()
        (acc_gate[e], acc_up[e]), ssq = take(tp, e)
        squares.append(ssq)
    combine[...] = (placing * weight).T

    for e in range(n_exp):
        ssq = squares[e]
        gate, up = acc_gate[e], acc_up[e]
        for hop in hops:
            j = partner(tp, hop, n_tp)
            if e == 0:
                for c in chips:
                    landed(rows.at[j, pl.ds(c * pair, pair)], gath_recv.at[j, c])
            (more_gate, more_up), more = take(j, e)
            gate, up, ssq = gate + more_gate, up + more_up, ssq + more
        factor = lax.rsqrt(ssq / width + norm_eps).reshape(n_ep * CAP, 1)
        finish(gate, up, factor, e)

    for e in range(n_exp):
        for step in reversed(range(n_chip)):
            c = chips[step]
            landed(part_in.at[e, c], part_recv.at[e, c])
            total = part[tp, pl.ds(c * pair, pair), e].astype(jnp.float32)
            for hop in hops:
                total = total + part_in[e, c, hop - 1].astype(jnp.float32)
            ret_out[pl.ds(c * pair, pair), e] = total.astype(jnp.bfloat16)
            group = peers[step * pair - 1 : (step + 1) * pair - 1] if step else peers[: pair - 1]
            for peer in group:
                give_back(peer, e).start()
            if not step:
                ret_in[ep, e] = ret_out[ep, e]

    both = combine[...]
    high = both.astype(jnp.bfloat16)
    low = (both - high.astype(jnp.float32)).astype(jnp.bfloat16)

    others = pl.ds(0, n_ep - 1)
    landed(outgoing.at[others], disp_send)
    landed(rows.at[pl.ds(0, n_tp - 1)], gath_send)
    landed(part.at[pl.ds(0, n_tp - 1)], part_send)
    landed(ret_in.at[others], ret_recv)
    back = ret_in[...].reshape(slots, cols)
    out_ref[...] = (
        jnp.dot(high, back, preferred_element_type=jnp.float32)
        + jnp.dot(low, back, preferred_element_type=jnp.float32)
    ).astype(jnp.bfloat16)
    landed(ret_out.at[others], ret_send)


def per_device(tokens, routing, gate_weights, norm_gain, w_gate, w_up, w_down):
    n_ep, n_tp = lax.axis_size("ep"), lax.axis_size("tp")
    n_exp, width, ff = w_gate.shape
    n_tok, cols = tokens.shape
    slots = n_ep * n_exp * CAP
    pair = 2 if n_ep % 2 == 0 else 1
    n_chip = n_ep // pair
    vmem = pl.BlockSpec(memory_space=pltpu.VMEM)
    hbm = pl.BlockSpec(memory_space=pltpu.HBM)
    bf16, f32 = jnp.bfloat16, jnp.float32
    dma = pltpu.SemaphoreType.DMA
    return pl.pallas_call(
        functools.partial(kernel, n_ep, n_tp),
        out_shape=pltpu.VMEM((n_tok, cols), bf16),
        in_specs=[hbm] * 7,
        out_specs=vmem,
        scratch_shapes=[
            pltpu.VMEM(tokens.shape, bf16),
            pltpu.VMEM(routing.shape[::-1], jnp.int32),
            pltpu.VMEM(gate_weights.shape[::-1], f32),
            pltpu.VMEM((1, width), f32),
            pltpu.VMEM(w_gate.shape, bf16),
            pltpu.VMEM(w_up.shape, bf16),
            pltpu.VMEM(w_down.shape, bf16),
            pltpu.VMEM((n_ep, n_exp, CAP, cols), bf16),
            pltpu.VMEM((n_tp, n_ep, n_exp, CAP, cols), bf16),
            pltpu.VMEM((n_tok, slots), f32),
            pltpu.VMEM((n_exp, n_ep * CAP, ff), f32),
            pltpu.VMEM((n_exp, n_ep * CAP, ff), f32),
            pltpu.VMEM((n_tp, n_ep, n_exp, CAP, cols), bf16),
            pltpu.VMEM((n_exp, n_chip, n_tp - 1, pair, CAP, cols), bf16),
            pltpu.VMEM((n_ep, n_exp, CAP, cols), bf16),
            pltpu.VMEM((n_ep, n_exp, CAP, cols), bf16),
            dma((4,)),
            dma((3, n_exp)),
            dma,
            dma((n_chip,)),
            dma,
            dma((n_tp, n_chip)),
            dma,
            dma((n_exp, n_chip)),
            dma,
            dma,
        ],
        compiler_params=pltpu.CompilerParams(collective_id=0, has_side_effects=True),
    )(tokens, routing.T, gate_weights.T, norm_gain.reshape(1, width), w_gate, w_up, w_down)


def solution(mesh):
    in_specs = (
        P("ep", "tp"),
        P("ep", None),
        P("ep", None),
        P(),
        P("ep", None, "tp"),
        P("ep", None, "tp"),
        P("ep", "tp", None),
    )
    return jax.shard_map(
        per_device, mesh=mesh, in_specs=in_specs, out_specs=P("ep", "tp"), check_vma=False
    )
```

```python
import functools

import jax
import jax.numpy as jnp
from jax import lax
from jax.experimental import pallas as pl
from jax.experimental.pallas import tpu as pltpu
from jax.sharding import PartitionSpec as P

CAP = 8
MESH = pl.DeviceIdType.MESH

norm_eps = 1e-06
clamp_limit = 7.0
swish_alpha = 1.702


def partner(me, step, n):
    if n & (n - 1):
        return lax.rem(me + step, n)
    other, bit = 0, 1
    while bit < n:
        mine = (me // bit) % 2
        other = other + bit * ((1 - mine) if step & bit else mine)
        bit *= 2
    return other


def nearest(me, step, n):
    bound = n * n
    found = 0
    for at in range(n):
        by_distance = sorted(range(n), key=lambda other: (abs(other - at), other))
        apart = (me - at) * (me - at)
        found = found + by_distance[step] * (1 - lax.div(apart + (bound - 1), bound))
    return found


def kernel(
    n_ep,
    n_tp,
    tok_hbm,
    rout_hbm,
    gw_hbm,
    gain_hbm,
    wg_hbm,
    wu_hbm,
    wd_hbm,
    out_ref,
    tok_ref,
    rout_ref,
    gw_ref,
    gain_ref,
    wg,
    wu,
    wd,
    outgoing,
    rows,
    combine,
    acc_gate,
    acc_up,
    part,
    part_in,
    ret_out,
    ret_in,
    in_sem,
    w_sem,
    disp_send,
    disp_recv,
    gath_send,
    gath_recv,
    part_send,
    part_recv,
    ret_send,
    ret_recv,
):
    ep, tp = lax.axis_index("ep"), lax.axis_index("tp")
    n_exp, width, ff = wg_hbm.shape
    n_tok, cols = tok_ref.shape
    top = rout_ref.shape[0]
    slots = n_ep * n_exp * CAP
    pair = 2 if n_ep % 2 == 0 else 1
    n_chip = n_ep // pair
    chip, core = lax.div(ep, pair), lax.rem(ep, pair)
    chips = [chip] + [nearest(chip, step, n_chip) for step in range(1, n_chip)]
    cores = [lax.rem(core + turn, pair) for turn in range(pair)]
    peers = [chips[0] * pair + k for k in cores[1:]]
    peers += [other * pair + k for other in chips[1:] for k in cores]
    hops = list(range(1, n_tp))

    small = [
        pltpu.make_async_copy(src, dst, in_sem.at[i])
        for i, (src, dst) in enumerate(
            ((rout_hbm, rout_ref), (gw_hbm, gw_ref), (tok_hbm, tok_ref), (gain_hbm, gain_ref))
        )
    ]
    for copy in small:
        copy.start()

    barrier = pltpu.get_barrier_semaphore()
    for peer in peers[::-1]:
        pl.semaphore_signal(barrier, inc=1, device_id=(peer, tp), device_id_type=MESH)
    for hop in hops[::-1]:
        pl.semaphore_signal(
            barrier, inc=1, device_id=(ep, partner(tp, hop, n_tp)), device_id_type=MESH
        )

    loads = []
    for e in range(n_exp):
        for i, (src, dst) in enumerate(((wg_hbm, wg), (wu_hbm, wu), (wd_hbm, wd))):
            loads.append(pltpu.make_async_copy(src.at[e], dst.at[e], w_sem.at[i, e]))
    for load in loads:
        load.start()

    slot = lax.broadcasted_iota(jnp.int32, (slots, n_tok), 0)
    group, slot_rank = slot // CAP, slot % CAP
    slot_exp = (group % n_ep) * n_exp + group // n_ep
    named = jnp.zeros((slots, n_tok), jnp.float32)
    weight = jnp.zeros((slots, n_tok), jnp.float32)
    earlier = jnp.where(
        lax.broadcasted_iota(jnp.int32, (n_tok, n_tok), 0)
        < lax.broadcasted_iota(jnp.int32, (n_tok, n_tok), 1),
        1.0,
        0.0,
    ).astype(jnp.bfloat16)
    small[0].wait()
    small[1].wait()
    for k in range(top):
        hit = rout_ref[k : k + 1, :] == slot_exp
        named = named + jnp.where(hit, 1.0, 0.0)
        weight = weight + jnp.where(hit, gw_ref[k : k + 1, :], 0.0)
    rank = jnp.dot(named.astype(jnp.bfloat16), earlier, preferred_element_type=jnp.float32)
    placing = jnp.where(rank == slot_rank.astype(jnp.float32), named, 0.0)
    small[2].wait()
    sent = jnp.dot(
        placing.astype(jnp.bfloat16), tok_ref[...], preferred_element_type=jnp.float32
    )
    outgoing[...] = sent.astype(jnp.bfloat16).reshape(n_exp, n_ep, CAP, cols)
    for e in range(n_exp):
        rows[tp, e, ep] = outgoing[e, ep]

    pl.semaphore_wait(barrier, n_ep - 1 + n_tp - 1)

    def dispatch(peer, e):
        return pltpu.make_async_remote_copy(
            src_ref=outgoing.at[e, peer],
            dst_ref=rows.at[tp, e, ep],
            send_sem=disp_send,
            recv_sem=disp_recv.at[e, chip],
            device_id=(peer, tp),
            device_id_type=MESH,
        )

    def gather(src, hop, e, s, count):
        return pltpu.make_async_remote_copy(
            src_ref=src,
            dst_ref=rows.at[tp, e, pl.ds(s, count)],
            send_sem=gath_send,
            recv_sem=gath_recv.at[e, tp],
            device_id=(ep, partner(tp, hop, n_tp)),
            device_id_type=MESH,
        )

    def reduce(hop, e, c):
        q = partner(tp, hop, n_tp)
        return pltpu.make_async_remote_copy(
            src_ref=part.at[q, e, pl.ds(c * pair, pair)],
            dst_ref=part_in.at[e, c, hop - 1],
            send_sem=part_send,
            recv_sem=part_recv.at[e, c],
            device_id=(ep, q),
            device_id_type=MESH,
        )

    def give_back(peer, e):
        return pltpu.make_async_remote_copy(
            src_ref=ret_out.at[e, peer],
            dst_ref=ret_in.at[e, ep],
            send_sem=ret_send,
            recv_sem=ret_recv,
            device_id=(peer, tp),
            device_id_type=MESH,
        )

    def landed(ref, sem):
        pltpu.make_async_copy(ref, ref, sem).wait()

    def piece(hidden, q, e):
        at = pl.multiple_of(q * cols, cols)
        part[q, e] = (
            jnp.dot(hidden, wd[e, :, pl.ds(at, cols)], preferred_element_type=jnp.float32)
            .reshape(n_ep, CAP, cols)
            .astype(jnp.bfloat16)
        )

    def finish(pre_gate, pre_up, factor, e):
        clamped = jnp.minimum(pre_gate * factor, clamp_limit)
        upper = jnp.clip(pre_up * factor, -clamp_limit, clamp_limit)
        hidden = (clamped * jax.nn.sigmoid(swish_alpha * clamped) * (upper + 1.0)).astype(
            jnp.bfloat16
        )
        loads[3 * e + 2].wait()
        if e < n_exp - 1:
            down = jnp.dot(hidden, wd[e], preferred_element_type=jnp.float32).astype(jnp.bfloat16)
            for q in range(n_tp):
                part[q, e] = down[:, q * cols : (q + 1) * cols].reshape(n_ep, CAP, cols)
        else:
            for hop in hops[::-1]:
                piece(hidden, partner(tp, hop, n_tp), e)
        for c in chips[:0:-1]:
            for hop in hops[::-1]:
                reduce(hop, e, c).start()
        if e == n_exp - 1:
            piece(hidden, tp, e)

    for e in range(n_exp):
        for peer in peers:
            dispatch(peer, e).start()
    for e in range(n_exp):
        for hop in hops[::-1]:
            gather(outgoing.at[e, pl.ds(ep, 1)], hop, e, ep, 1).start()

    def take(j, e):
        wide = rows[j, e].astype(jnp.float32)
        at = pl.multiple_of(j * cols, cols)
        x = wide * gain_ref[:, pl.ds(at, cols)].reshape(1, 1, cols)
        x = x.reshape(n_ep * CAP, cols).astype(jnp.bfloat16)
        y = [
            jnp.dot(x, w[e, pl.ds(at, cols), :], preferred_element_type=jnp.float32)
            for w in (wg, wu)
        ]
        return y, jnp.sum(wide * wide, axis=2, keepdims=True)

    squares = []
    for e in range(n_exp):
        for s in peers[: pair - 1]:
            landed(rows.at[tp, e, s], disp_recv.at[e, chip])
            for hop in hops[::-1]:
                gather(rows.at[tp, e, pl.ds(s, 1)], hop, e, s, 1).start()
        for c in chips[1:]:
            here = rows.at[tp, e, pl.ds(c * pair, pair)]
            landed(here, disp_recv.at[e, c])
            for hop in hops[::-1]:
                gather(here, hop, e, c * pair, pair).start()
        if not e:
            small[3].wait()
        loads[3 * e].wait()
        loads[3 * e + 1].wait()
        (acc_gate[e], acc_up[e]), ssq = take(tp, e)
        squares.append(ssq)
    combine[...] = (placing * weight).T

    for e in range(n_exp):
        ssq = squares[e]
        gate, up = acc_gate[e], acc_up[e]
        for hop in hops:
            j = partner(tp, hop, n_tp)
            landed(rows.at[j, e], gath_recv.at[e, j])
            (more_gate, more_up), more = take(j, e)
            gate, up, ssq = gate + more_gate, up + more_up, ssq + more
        factor = lax.rsqrt(ssq / width + norm_eps).reshape(n_ep * CAP, 1)
        finish(gate, up, factor, e)
    for e in range(n_exp):
        for hop in hops[::-1]:
            reduce(hop, e, chip).start()

    turns = [(e, step) for e in range(n_exp) for step in range(n_chip - 1, 0, -1)]
    turns += [(e, 0) for e in range(n_exp)]
    for e, step in turns:
        c = chips[step]
        landed(part_in.at[e, c], part_recv.at[e, c])
        total = part[tp, e, pl.ds(c * pair, pair)].astype(jnp.float32)
        for hop in hops:
            total = total + part_in[e, c, hop - 1].astype(jnp.float32)
        ret_out[e, pl.ds(c * pair, pair)] = total.astype(jnp.bfloat16)
        group = peers[step * pair - 1 : (step + 1) * pair - 1] if step else peers[: pair - 1]
        for peer in group:
            give_back(peer, e).start()
        if not step:
            ret_in[e, ep] = ret_out[e, ep]

    both = combine[...]
    high = both.astype(jnp.bfloat16)
    low = (both - high.astype(jnp.float32)).astype(jnp.bfloat16)

    others = pl.ds(0, n_ep - 1)
    landed(outgoing.at[:, others], disp_send)
    landed(rows.at[pl.ds(0, n_tp - 1)], gath_send)
    landed(part.at[pl.ds(0, n_tp - 1)], part_send)
    landed(ret_in.at[:, others], ret_recv)
    back = ret_in[...].reshape(slots, cols)
    out_ref[...] = (
        jnp.dot(high, back, preferred_element_type=jnp.float32)
        + jnp.dot(low, back, preferred_element_type=jnp.float32)
    ).astype(jnp.bfloat16)
    landed(ret_out.at[:, others], ret_send)


def per_device(tokens, routing, gate_weights, norm_gain, w_gate, w_up, w_down):
    n_ep, n_tp = lax.axis_size("ep"), lax.axis_size("tp")
    n_exp, width, ff = w_gate.shape
    n_tok, cols = tokens.shape
    slots = n_ep * n_exp * CAP
    pair = 2 if n_ep % 2 == 0 else 1
    n_chip = n_ep // pair
    vmem = pl.BlockSpec(memory_space=pltpu.VMEM)
    hbm = pl.BlockSpec(memory_space=pltpu.HBM)
    bf16, f32 = jnp.bfloat16, jnp.float32
    dma = pltpu.SemaphoreType.DMA
    return pl.pallas_call(
        functools.partial(kernel, n_ep, n_tp),
        out_shape=pltpu.VMEM((n_tok, cols), bf16),
        in_specs=[hbm] * 7,
        out_specs=vmem,
        scratch_shapes=[
            pltpu.VMEM(tokens.shape, bf16),
            pltpu.VMEM(routing.shape[::-1], jnp.int32),
            pltpu.VMEM(gate_weights.shape[::-1], f32),
            pltpu.VMEM((1, width), f32),
            pltpu.VMEM(w_gate.shape, bf16),
            pltpu.VMEM(w_up.shape, bf16),
            pltpu.VMEM(w_down.shape, bf16),
            pltpu.VMEM((n_exp, n_ep, CAP, cols), bf16),
            pltpu.VMEM((n_tp, n_exp, n_ep, CAP, cols), bf16),
            pltpu.VMEM((n_tok, slots), f32),
            pltpu.VMEM((n_exp, n_ep * CAP, ff), f32),
            pltpu.VMEM((n_exp, n_ep * CAP, ff), f32),
            pltpu.VMEM((n_tp, n_exp, n_ep, CAP, cols), bf16),
            pltpu.VMEM((n_exp, n_chip, n_tp - 1, pair, CAP, cols), bf16),
            pltpu.VMEM((n_exp, n_ep, CAP, cols), bf16),
            pltpu.VMEM((n_exp, n_ep, CAP, cols), bf16),
            dma((4,)),
            dma((3, n_exp)),
            dma,
            dma((n_exp, n_chip)),
            dma,
            dma((n_exp, n_tp)),
            dma,
            dma((n_exp, n_chip)),
            dma,
            dma,
        ],
        compiler_params=pltpu.CompilerParams(collective_id=0, has_side_effects=True),
    )(tokens, routing.T, gate_weights.T, norm_gain.reshape(1, width), w_gate, w_up, w_down)


def solution(mesh):
    in_specs = (
        P("ep", "tp"),
        P("ep", None),
        P("ep", None),
        P(),
        P("ep", None, "tp"),
        P("ep", None, "tp"),
        P("ep", "tp", None),
    )
    return jax.shard_map(
        per_device, mesh=mesh, in_specs=in_specs, out_specs=P("ep", "tp"), check_vma=False
    )
```

```python
import functools

import jax
import jax.numpy as jnp
from jax import lax
from jax.experimental import pallas as pl
from jax.experimental.pallas import tpu as pltpu
from jax.sharding import PartitionSpec as P

CAP = 8
MESH = pl.DeviceIdType.MESH

norm_eps = 1e-06
clamp_limit = 7.0
swish_alpha = 1.702


def partner(me, step, n):
    if n & (n - 1):
        return lax.rem(me + step, n)
    other, bit = 0, 1
    while bit < n:
        mine = (me // bit) % 2
        other = other + bit * ((1 - mine) if step & bit else mine)
        bit *= 2
    return other


def nearest(me, step, n):
    bound = n * n
    found = 0
    for at in range(n):
        by_distance = sorted(range(n), key=lambda other: (abs(other - at), other))
        apart = (me - at) * (me - at)
        found = found + by_distance[step] * (1 - lax.div(apart + (bound - 1), bound))
    return found


def kernel(
    n_ep,
    n_tp,
    tok_hbm,
    rout_hbm,
    gw_hbm,
    gain_hbm,
    wg_hbm,
    wu_hbm,
    wd_hbm,
    out_ref,
    tok_ref,
    rout_ref,
    gw_ref,
    gain_ref,
    wg,
    wu,
    wd,
    outgoing,
    rows,
    combine,
    acc_gate,
    acc_up,
    part,
    part_in,
    ret_out,
    ret_in,
    in_sem,
    w_sem,
    disp_send,
    disp_recv,
    gath_send,
    gath_recv,
    part_send,
    part_recv,
    ret_send,
    ret_recv,
    turn,
):
    ep, tp = lax.axis_index("ep"), lax.axis_index("tp")
    n_exp, width, ff = wg_hbm.shape
    n_tok, cols = tok_ref.shape
    top = rout_ref.shape[0]
    slots = n_ep * n_exp * CAP
    pair = 2 if n_ep % 2 == 0 else 1
    n_chip = n_ep // pair
    chip, core = lax.div(ep, pair), lax.rem(ep, pair)
    chips = [chip] + [nearest(chip, step, n_chip) for step in range(1, n_chip)]
    cores = [lax.rem(core + turn, pair) for turn in range(pair)]
    peers = [chips[0] * pair + k for k in cores[1:]]
    peers += [other * pair + k for other in chips[1:] for k in cores]
    hops = list(range(1, n_tp))

    small = [
        pltpu.make_async_copy(src, dst, in_sem.at[i])
        for i, (src, dst) in enumerate(
            ((rout_hbm, rout_ref), (gw_hbm, gw_ref), (tok_hbm, tok_ref), (gain_hbm, gain_ref))
        )
    ]
    for copy in small:
        copy.start()

    barrier = pltpu.get_barrier_semaphore()
    for peer in peers[::-1]:
        pl.semaphore_signal(barrier, inc=1, device_id=(peer, tp), device_id_type=MESH)
    for hop in hops[::-1]:
        pl.semaphore_signal(
            barrier, inc=1, device_id=(ep, partner(tp, hop, n_tp)), device_id_type=MESH
        )

    loads = []
    for e in range(n_exp):
        for i, (src, dst) in enumerate(((wg_hbm, wg), (wu_hbm, wu), (wd_hbm, wd))):
            loads.append(pltpu.make_async_copy(src.at[e], dst.at[e], w_sem.at[i, e]))
    for load in loads:
        load.start()

    slot = lax.broadcasted_iota(jnp.int32, (slots, n_tok), 0)
    group, slot_rank = slot // CAP, slot % CAP
    slot_exp = (group % n_ep) * n_exp + group // n_ep
    named = jnp.zeros((slots, n_tok), jnp.float32)
    weight = jnp.zeros((slots, n_tok), jnp.float32)
    earlier = jnp.where(
        lax.broadcasted_iota(jnp.int32, (n_tok, n_tok), 0)
        < lax.broadcasted_iota(jnp.int32, (n_tok, n_tok), 1),
        1.0,
        0.0,
    ).astype(jnp.bfloat16)
    small[0].wait()
    small[1].wait()
    for k in range(top):
        hit = rout_ref[k : k + 1, :] == slot_exp
        named = named + jnp.where(hit, 1.0, 0.0)
        weight = weight + jnp.where(hit, gw_ref[k : k + 1, :], 0.0)
    rank = jnp.dot(named.astype(jnp.bfloat16), earlier, preferred_element_type=jnp.float32)
    placing = jnp.where(rank == slot_rank.astype(jnp.float32), named, 0.0)
    small[2].wait()
    sent = jnp.dot(
        placing.astype(jnp.bfloat16), tok_ref[...], preferred_element_type=jnp.float32
    )
    outgoing[...] = sent.astype(jnp.bfloat16).reshape(n_exp, n_ep, CAP, cols)
    for e in range(n_exp):
        rows[tp, e, ep] = outgoing[e, ep]

    pl.semaphore_wait(barrier, n_ep - 1 + n_tp - 1)

    def dispatch(peer, e):
        return pltpu.make_async_remote_copy(
            src_ref=outgoing.at[e, peer],
            dst_ref=rows.at[tp, e, ep],
            send_sem=disp_send,
            recv_sem=disp_recv.at[e, chip],
            device_id=(peer, tp),
            device_id_type=MESH,
        )

    def gather(src, hop, e, s, count):
        return pltpu.make_async_remote_copy(
            src_ref=src,
            dst_ref=rows.at[tp, e, pl.ds(s, count)],
            send_sem=gath_send,
            recv_sem=gath_recv.at[e, tp],
            device_id=(ep, partner(tp, hop, n_tp)),
            device_id_type=MESH,
        )

    def reduce(hop, e, c):
        q = partner(tp, hop, n_tp)
        return pltpu.make_async_remote_copy(
            src_ref=part.at[q, e, pl.ds(c * pair, pair)],
            dst_ref=part_in.at[e, c, hop - 1],
            send_sem=part_send,
            recv_sem=part_recv.at[e, c],
            device_id=(ep, q),
            device_id_type=MESH,
        )

    def give_back(peer, e):
        return pltpu.make_async_remote_copy(
            src_ref=ret_out.at[e, peer],
            dst_ref=ret_in.at[e, ep],
            send_sem=ret_send,
            recv_sem=ret_recv,
            device_id=(peer, tp),
            device_id_type=MESH,
        )

    def landed(ref, sem):
        pltpu.make_async_copy(ref, ref, sem).wait()

    def piece(hidden, q, e):
        at = pl.multiple_of(q * cols, cols)
        part[q, e] = (
            jnp.dot(hidden, wd[e, :, pl.ds(at, cols)], preferred_element_type=jnp.float32)
            .reshape(n_ep, CAP, cols)
            .astype(jnp.bfloat16)
        )

    def finish(pre_gate, pre_up, factor, e):
        clamped = jnp.minimum(pre_gate * factor, clamp_limit)
        upper = jnp.clip(pre_up * factor, -clamp_limit, clamp_limit)
        hidden = (clamped * jax.nn.sigmoid(swish_alpha * clamped) * (upper + 1.0)).astype(
            jnp.bfloat16
        )
        loads[3 * e + 2].wait()
        for hop in hops[::-1]:
            piece(hidden, partner(tp, hop, n_tp), e)
            if e < n_exp - 1:
                for c in chips[:0:-1]:
                    reduce(hop, e, c).start()
        if e == n_exp - 1:
            for c in chips[:0:-1]:
                for hop in hops[::-1]:
                    reduce(hop, e, c).start()
        piece(hidden, tp, e)

    for e in range(n_exp):
        for k in cores[1:]:
            dispatch(chip * pair + k, e).start()
        for other in chips[1:]:
            for k in range(pair):
                dispatch(other * pair + k, e).start()
    for e in range(n_exp):
        for hop in hops[::-1]:
            gather(outgoing.at[e, pl.ds(ep, 1)], hop, e, ep, 1).start()

    def take(j, e):
        wide = rows[j, e].astype(jnp.float32)
        at = pl.multiple_of(j * cols, cols)
        x = wide * gain_ref[:, pl.ds(at, cols)].reshape(1, 1, cols)
        x = x.reshape(n_ep * CAP, cols).astype(jnp.bfloat16)
        y = [
            jnp.dot(x, w[e, pl.ds(at, cols), :], preferred_element_type=jnp.float32)
            for w in (wg, wu)
        ]
        return y, jnp.sum(wide * wide, axis=2, keepdims=True)

    def forward(turns):
        for e, step in turns:
            c = chips[step]
            if step == 0:
                for s in peers[: pair - 1]:
                    landed(rows.at[tp, e, s], disp_recv.at[e, c])
                    for hop in hops[::-1]:
                        gather(rows.at[tp, e, pl.ds(s, 1)], hop, e, s, 1).start()
            else:
                here = rows.at[tp, e, pl.ds(c * pair, pair)]
                landed(here, disp_recv.at[e, c])
                for hop in hops[::-1]:
                    gather(here, hop, e, c * pair, pair).start()

    soon = [(e, 0) for e in range(n_exp)] + [(0, step) for step in range(1, n_chip)]
    later = [(e, step) for e in range(1, n_exp) for step in range(1, n_chip)]
    forward(soon)
    if pair == 2:

        @pl.when(core == 0)
        def _():
            forward(later)
            pl.semaphore_signal(turn, inc=1, device_id=(ep + 1, tp), device_id_type=MESH)

        @pl.when(core != 0)
        def _():
            pl.semaphore_wait(turn, 1)
            forward(later)

    else:
        forward(later)
    squares = []
    small[3].wait()
    for e in range(n_exp):
        loads[3 * e].wait()
        loads[3 * e + 1].wait()
        (acc_gate[e], acc_up[e]), ssq = take(tp, e)
        squares.append(ssq)
    combine[...] = (placing * weight).T

    for e in range(n_exp):
        ssq = squares[e]
        gate, up = acc_gate[e], acc_up[e]
        for hop in hops:
            j = partner(tp, hop, n_tp)
            landed(rows.at[j, e], gath_recv.at[e, j])
            (more_gate, more_up), more = take(j, e)
            gate, up, ssq = gate + more_gate, up + more_up, ssq + more
        factor = lax.rsqrt(ssq / width + norm_eps).reshape(n_ep * CAP, 1)
        finish(gate, up, factor, e)
    for e in range(n_exp):
        for hop in hops[::-1]:
            reduce(hop, e, chip).start()

    turns = [(e, step) for e in range(n_exp) for step in range(n_chip - 1, 0, -1)]
    turns += [(e, 0) for e in range(n_exp)]
    for e, step in turns:
        c = chips[step]
        landed(part_in.at[e, c], part_recv.at[e, c])
        total = part[tp, e, pl.ds(c * pair, pair)].astype(jnp.float32)
        for hop in hops:
            total = total + part_in[e, c, hop - 1].astype(jnp.float32)
        ret_out[e, pl.ds(c * pair, pair)] = total.astype(jnp.bfloat16)
        group = peers[step * pair - 1 : (step + 1) * pair - 1] if step else peers[: pair - 1]
        for peer in group:
            give_back(peer, e).start()
        if not step:
            ret_in[e, ep] = ret_out[e, ep]

    both = combine[...]
    high = both.astype(jnp.bfloat16)
    low = (both - high.astype(jnp.float32)).astype(jnp.bfloat16)

    others = pl.ds(0, n_ep - 1)
    landed(outgoing.at[:, others], disp_send)
    landed(rows.at[pl.ds(0, n_tp - 1)], gath_send)
    landed(part.at[pl.ds(0, n_tp - 1)], part_send)
    landed(ret_in.at[:, others], ret_recv)
    back = ret_in[...].reshape(slots, cols)
    out_ref[...] = (
        jnp.dot(high, back, preferred_element_type=jnp.float32)
        + jnp.dot(low, back, preferred_element_type=jnp.float32)
    ).astype(jnp.bfloat16)
    landed(ret_out.at[:, others], ret_send)


def per_device(tokens, routing, gate_weights, norm_gain, w_gate, w_up, w_down):
    n_ep, n_tp = lax.axis_size("ep"), lax.axis_size("tp")
    n_exp, width, ff = w_gate.shape
    n_tok, cols = tokens.shape
    slots = n_ep * n_exp * CAP
    pair = 2 if n_ep % 2 == 0 else 1
    n_chip = n_ep // pair
    vmem = pl.BlockSpec(memory_space=pltpu.VMEM)
    hbm = pl.BlockSpec(memory_space=pltpu.HBM)
    bf16, f32 = jnp.bfloat16, jnp.float32
    dma = pltpu.SemaphoreType.DMA
    return pl.pallas_call(
        functools.partial(kernel, n_ep, n_tp),
        out_shape=pltpu.VMEM((n_tok, cols), bf16),
        in_specs=[hbm] * 7,
        out_specs=vmem,
        scratch_shapes=[
            pltpu.VMEM(tokens.shape, bf16),
            pltpu.VMEM(routing.shape[::-1], jnp.int32),
            pltpu.VMEM(gate_weights.shape[::-1], f32),
            pltpu.VMEM((1, width), f32),
            pltpu.VMEM(w_gate.shape, bf16),
            pltpu.VMEM(w_up.shape, bf16),
            pltpu.VMEM(w_down.shape, bf16),
            pltpu.VMEM((n_exp, n_ep, CAP, cols), bf16),
            pltpu.VMEM((n_tp, n_exp, n_ep, CAP, cols), bf16),
            pltpu.VMEM((n_tok, slots), f32),
            pltpu.VMEM((n_exp, n_ep * CAP, ff), f32),
            pltpu.VMEM((n_exp, n_ep * CAP, ff), f32),
            pltpu.VMEM((n_tp, n_exp, n_ep, CAP, cols), bf16),
            pltpu.VMEM((n_exp, n_chip, n_tp - 1, pair, CAP, cols), bf16),
            pltpu.VMEM((n_exp, n_ep, CAP, cols), bf16),
            pltpu.VMEM((n_exp, n_ep, CAP, cols), bf16),
            dma((4,)),
            dma((3, n_exp)),
            dma,
            dma((n_exp, n_chip)),
            dma,
            dma((n_exp, n_tp)),
            dma,
            dma((n_exp, n_chip)),
            dma,
            dma,
            pltpu.SemaphoreType.REGULAR,
        ],
        compiler_params=pltpu.CompilerParams(collective_id=0, has_side_effects=True),
    )(tokens, routing.T, gate_weights.T, norm_gain.reshape(1, width), w_gate, w_up, w_down)


def solution(mesh):
    in_specs = (
        P("ep", "tp"),
        P("ep", None),
        P("ep", None),
        P(),
        P("ep", None, "tp"),
        P("ep", None, "tp"),
        P("ep", "tp", None),
    )
    return jax.shard_map(
        per_device, mesh=mesh, in_specs=in_specs, out_specs=P("ep", "tp"), check_vma=False
    )
```

```python
import functools

import jax
import jax.numpy as jnp
from jax import lax
from jax.experimental import pallas as pl
from jax.experimental.pallas import tpu as pltpu
from jax.sharding import PartitionSpec as P

CAP = 8
MESH = pl.DeviceIdType.MESH

norm_eps = 1e-06
clamp_limit = 7.0
swish_alpha = 1.702


def partner(me, step, n):
    if n & (n - 1):
        return lax.rem(me + step, n)
    other, bit = 0, 1
    while bit < n:
        mine = (me // bit) % 2
        other = other + bit * ((1 - mine) if step & bit else mine)
        bit *= 2
    return other


def nearest(me, step, n):
    bound = n * n
    found = 0
    for at in range(n):
        by_distance = sorted(range(n), key=lambda other: (abs(other - at), other))
        apart = (me - at) * (me - at)
        found = found + by_distance[step] * (1 - lax.div(apart + (bound - 1), bound))
    return found


def kernel(
    n_ep,
    n_tp,
    tok_hbm,
    rout_hbm,
    gw_hbm,
    gain_hbm,
    wg_hbm,
    wu_hbm,
    wd_hbm,
    out_ref,
    tok_ref,
    rout_ref,
    gw_ref,
    gain_ref,
    wgu,
    wd,
    outgoing,
    rows,
    combine,
    acc_gate,
    acc_up,
    part,
    part_in,
    ret_out,
    ret_in,
    in_sem,
    gu_sem,
    down_sem,
    row_send,
    disp_recv,
    gath_send,
    gath_recv,
    part_send,
    part_recv,
    ret_recv,
    turn,
):
    ep, tp = lax.axis_index("ep"), lax.axis_index("tp")
    n_exp, width, ff = wg_hbm.shape
    n_tok, cols = tok_ref.shape
    top = rout_ref.shape[0]
    slots = n_ep * n_exp * CAP
    pair = 2 if n_ep % 2 == 0 else 1
    n_chip = n_ep // pair
    chip, core = lax.div(ep, pair), lax.rem(ep, pair)
    chips = [chip] + [nearest(chip, step, n_chip) for step in range(1, n_chip)]
    cores = [lax.rem(core + turn, pair) for turn in range(pair)]
    peers = [chips[0] * pair + k for k in cores[1:]]
    peers += [other * pair + k for other in chips[1:] for k in cores]
    hops = list(range(1, n_tp))

    small = [
        pltpu.make_async_copy(src, dst, in_sem.at[i])
        for i, (src, dst) in enumerate(
            ((rout_hbm, rout_ref), (gw_hbm, gw_ref), (tok_hbm, tok_ref), (gain_hbm, gain_ref))
        )
    ]
    for copy in small:
        copy.start()

    barrier = pltpu.get_barrier_semaphore()
    for peer in peers[::-1]:
        pl.semaphore_signal(barrier, inc=1, device_id=(peer, tp), device_id_type=MESH)
    for hop in hops[::-1]:
        pl.semaphore_signal(
            barrier, inc=1, device_id=(ep, partner(tp, hop, n_tp)), device_id_type=MESH
        )

    loads = []
    for e in range(n_exp):
        loads.append(pltpu.make_async_copy(wg_hbm.at[e], wgu.at[0, e], gu_sem))
        loads.append(pltpu.make_async_copy(wu_hbm.at[e], wgu.at[1, e], gu_sem))
    for load in loads:
        load.start()
    down_load = pltpu.make_async_copy(wd_hbm, wd, down_sem)
    down_load.start()

    slot = lax.broadcasted_iota(jnp.int32, (slots, n_tok), 0)
    group, slot_rank = slot // CAP, slot % CAP
    slot_exp = (group % n_ep) * n_exp + group // n_ep
    named = jnp.zeros((slots, n_tok), jnp.float32)
    weight = jnp.zeros((slots, n_tok), jnp.float32)
    earlier = jnp.where(
        lax.broadcasted_iota(jnp.int32, (n_tok, n_tok), 0)
        < lax.broadcasted_iota(jnp.int32, (n_tok, n_tok), 1),
        1.0,
        0.0,
    ).astype(jnp.bfloat16)
    small[0].wait()
    small[1].wait()
    for k in range(top):
        hit = rout_ref[k : k + 1, :] == slot_exp
        named = named + jnp.where(hit, 1.0, 0.0)
        weight = weight + jnp.where(hit, gw_ref[k : k + 1, :], 0.0)
    rank = jnp.dot(named.astype(jnp.bfloat16), earlier, preferred_element_type=jnp.float32)
    placing = jnp.where(rank == slot_rank.astype(jnp.float32), named, 0.0)
    small[2].wait()
    sent = jnp.dot(
        placing.astype(jnp.bfloat16), tok_ref[...], preferred_element_type=jnp.float32
    )
    outgoing[...] = sent.astype(jnp.bfloat16).reshape(n_exp, n_ep, CAP, cols)
    for e in range(n_exp):
        rows[tp, e, ep] = outgoing[e, ep]

    pl.semaphore_wait(barrier, n_ep - 1 + n_tp - 1)

    def dispatch(peer, e):
        return pltpu.make_async_remote_copy(
            src_ref=outgoing.at[e, peer],
            dst_ref=rows.at[tp, e, ep],
            send_sem=row_send,
            recv_sem=disp_recv.at[e, chip],
            device_id=(peer, tp),
            device_id_type=MESH,
        )

    def gather(src, hop, e, s, count):
        return pltpu.make_async_remote_copy(
            src_ref=src,
            dst_ref=rows.at[tp, e, pl.ds(s, count)],
            send_sem=gath_send,
            recv_sem=gath_recv.at[e, hop - 1],
            device_id=(ep, partner(tp, hop, n_tp)),
            device_id_type=MESH,
        )

    def reduce(hop, e, c):
        q = partner(tp, hop, n_tp)
        return pltpu.make_async_remote_copy(
            src_ref=part.at[q, e, pl.ds(c * pair, pair)],
            dst_ref=part_in.at[e, c, hop - 1],
            send_sem=part_send,
            recv_sem=part_recv.at[e, c],
            device_id=(ep, q),
            device_id_type=MESH,
        )

    def give_back(peer, e):
        return pltpu.make_async_remote_copy(
            src_ref=ret_out.at[e, peer],
            dst_ref=ret_in.at[e, ep],
            send_sem=row_send,
            recv_sem=ret_recv,
            device_id=(peer, tp),
            device_id_type=MESH,
        )

    def landed(ref, sem):
        pltpu.make_async_copy(ref, ref, sem).wait()

    def piece(hidden, q, e):
        at = pl.multiple_of(q * cols, cols)
        part[q, e] = (
            jnp.dot(hidden, wd[e, :, pl.ds(at, cols)], preferred_element_type=jnp.float32)
            .reshape(n_ep, CAP, cols)
            .astype(jnp.bfloat16)
        )

    def finish(pre_gate, pre_up, factor, e):
        clamped = jnp.minimum(pre_gate * factor, clamp_limit)
        upper = jnp.clip(pre_up * factor, -clamp_limit, clamp_limit)
        hidden = (clamped * jax.nn.sigmoid(swish_alpha * clamped) * (upper + 1.0)).astype(
            jnp.bfloat16
        )
        if not e:
            down_load.wait()
        for hop in hops[::-1]:
            piece(hidden, partner(tp, hop, n_tp), e)
            if e < n_exp - 1:
                for c in chips[:0:-1]:
                    reduce(hop, e, c).start()
        if e == n_exp - 1:
            for c in chips[:0:-1]:
                for hop in hops[::-1]:
                    reduce(hop, e, c).start()
        piece(hidden, tp, e)

    for e in range(n_exp):
        for k in cores[1:]:
            dispatch(chip * pair + k, e).start()
        for other in chips[1:]:
            for k in range(pair):
                dispatch(other * pair + k, e).start()
    for e in range(n_exp):
        for hop in hops[::-1]:
            gather(outgoing.at[e, pl.ds(ep, 1)], hop, e, ep, 1).start()

    def take(j, e):
        wide = rows[j, e].astype(jnp.float32)
        at = pl.multiple_of(j * cols, cols)
        x = wide * gain_ref[:, pl.ds(at, cols)].reshape(1, 1, cols)
        x = x.reshape(n_ep * CAP, cols).astype(jnp.bfloat16)
        y = [
            jnp.dot(x, wgu[i, e, pl.ds(at, cols), :], preferred_element_type=jnp.float32)
            for i in range(2)
        ]
        return y, jnp.sum(wide * wide, axis=2, keepdims=True)

    def forward(turns, await_rows=True, send=True):
        for e, step in turns:
            c = chips[step]
            if step == 0:
                for s in peers[: pair - 1]:
                    landed(rows.at[tp, e, s], disp_recv.at[e, c])
                    for hop in hops[::-1]:
                        gather(rows.at[tp, e, pl.ds(s, 1)], hop, e, s, 1).start()
            else:
                here = rows.at[tp, e, pl.ds(c * pair, pair)]
                if await_rows:
                    landed(here, disp_recv.at[e, c])
                if send:
                    for hop in hops[::-1]:
                        gather(here, hop, e, c * pair, pair).start()

    soon = [(e, 0) for e in range(n_exp)] + [(0, step) for step in range(1, n_chip)]
    later = [(e, step) for e in range(1, n_exp) for step in range(1, n_chip)]
    forward(soon)
    if pair == 2:
        pl.when(core == 0)(lambda: forward(later))
        pl.when(core != 0)(lambda: forward(later, send=False))
    else:
        forward(later)
    squares = []
    small[3].wait()
    landed(wgu, gu_sem)
    for e in range(n_exp):
        (acc_gate[e], acc_up[e]), ssq = take(tp, e)
        squares.append(ssq)
    if pair == 2:

        @pl.when(core == 0)
        def _():
            pl.semaphore_signal(turn, inc=1, device_id=(ep + 1, tp), device_id_type=MESH)

        @pl.when(core != 0)
        def _():
            pl.semaphore_wait(turn, 1)
            forward(later, await_rows=False)

    combine[...] = (placing * weight).T

    for e in range(n_exp):
        ssq = squares[e]
        gate, up = acc_gate[e], acc_up[e]
        for hop in hops:
            j = partner(tp, hop, n_tp)
            landed(rows.at[j, e], gath_recv.at[e, (hop if n_tp & (n_tp - 1) == 0 else n_tp - hop) - 1])
            (more_gate, more_up), more = take(j, e)
            gate, up, ssq = gate + more_gate, up + more_up, ssq + more
        factor = lax.rsqrt(ssq / width + norm_eps).reshape(n_ep * CAP, 1)
        finish(gate, up, factor, e)
    for e in range(n_exp):
        for hop in hops[::-1]:
            reduce(hop, e, chip).start()

    turns = [(e, step) for e in range(n_exp) for step in range(n_chip - 1, 0, -1)]
    turns += [(e, 0) for e in range(n_exp)]
    for e, step in turns:
        c = chips[step]
        landed(part_in.at[e, c], part_recv.at[e, c])
        total = part[tp, e, pl.ds(c * pair, pair)].astype(jnp.float32)
        for hop in hops:
            total = total + part_in[e, c, hop - 1].astype(jnp.float32)
        ret_out[e, pl.ds(c * pair, pair)] = total.astype(jnp.bfloat16)
        group = peers[step * pair - 1 : (step + 1) * pair - 1] if step else peers[: pair - 1]
        for peer in group:
            give_back(peer, e).start()
        if not step:
            ret_in[e, ep] = ret_out[e, ep]

    both = combine[...]
    high = both.astype(jnp.bfloat16)
    low = (both - high.astype(jnp.float32)).astype(jnp.bfloat16)

    others = pl.ds(0, n_ep - 1)
    landed(rows.at[pl.ds(0, n_tp - 1)], gath_send)
    landed(part.at[pl.ds(0, n_tp - 1)], part_send)
    landed(ret_in.at[:, others], ret_recv)
    back = ret_in[...].reshape(slots, cols)
    out_ref[...] = (
        jnp.dot(high, back, preferred_element_type=jnp.float32)
        + jnp.dot(low, back, preferred_element_type=jnp.float32)
    ).astype(jnp.bfloat16)
    landed(rows.at[pl.ds(0, 2), :, others], row_send)


def per_device(tokens, routing, gate_weights, norm_gain, w_gate, w_up, w_down):
    n_ep, n_tp = lax.axis_size("ep"), lax.axis_size("tp")
    n_exp, width, ff = w_gate.shape
    n_tok, cols = tokens.shape
    slots = n_ep * n_exp * CAP
    pair = 2 if n_ep % 2 == 0 else 1
    n_chip = n_ep // pair
    vmem = pl.BlockSpec(memory_space=pltpu.VMEM)
    hbm = pl.BlockSpec(memory_space=pltpu.HBM)
    bf16, f32 = jnp.bfloat16, jnp.float32
    dma = pltpu.SemaphoreType.DMA
    return pl.pallas_call(
        functools.partial(kernel, n_ep, n_tp),
        out_shape=pltpu.VMEM((n_tok, cols), bf16),
        in_specs=[hbm] * 7,
        out_specs=vmem,
        scratch_shapes=[
            pltpu.VMEM(tokens.shape, bf16),
            pltpu.VMEM(routing.shape[::-1], jnp.int32),
            pltpu.VMEM(gate_weights.shape[::-1], f32),
            pltpu.VMEM((1, width), f32),
            pltpu.VMEM((2, *w_gate.shape), bf16),
            pltpu.VMEM(w_down.shape, bf16),
            pltpu.VMEM((n_exp, n_ep, CAP, cols), bf16),
            pltpu.VMEM((n_tp, n_exp, n_ep, CAP, cols), bf16),
            pltpu.VMEM((n_tok, slots), f32),
            pltpu.VMEM((n_exp, n_ep * CAP, ff), f32),
            pltpu.VMEM((n_exp, n_ep * CAP, ff), f32),
            pltpu.VMEM((n_tp, n_exp, n_ep, CAP, cols), bf16),
            pltpu.VMEM((n_exp, n_chip, n_tp - 1, pair, CAP, cols), bf16),
            pltpu.VMEM((n_exp, n_ep, CAP, cols), bf16),
            pltpu.VMEM((n_exp, n_ep, CAP, cols), bf16),
            dma((4,)),
            dma,
            dma,
            dma,
            dma((n_exp, n_chip)),
            dma,
            dma((n_exp, n_tp - 1)),
            dma,
            dma((n_exp, n_chip)),
            dma,
            pltpu.SemaphoreType.REGULAR,
        ],
        compiler_params=pltpu.CompilerParams(collective_id=0, has_side_effects=True),
    )(tokens, routing.T, gate_weights.T, norm_gain.reshape(1, width), w_gate, w_up, w_down)


def solution(mesh):
    in_specs = (
        P("ep", "tp"),
        P("ep", None),
        P("ep", None),
        P(),
        P("ep", None, "tp"),
        P("ep", None, "tp"),
        P("ep", "tp", None),
    )
    return jax.shard_map(
        per_device, mesh=mesh, in_specs=in_specs, out_specs=P("ep", "tp"), check_vma=False
    )
```

```python
import functools

import jax
import jax.numpy as jnp
from jax import lax
from jax.experimental import pallas as pl
from jax.experimental.pallas import tpu as pltpu
from jax.sharding import PartitionSpec as P

CAP = 8
MESH = pl.DeviceIdType.MESH

norm_eps = 1e-06
clamp_limit = 7.0
swish_alpha = 1.702


def partner(me, step, n):
    if n & (n - 1):
        return lax.rem(me + step, n)
    other, bit = 0, 1
    while bit < n:
        mine = (me // bit) % 2
        other = other + bit * ((1 - mine) if step & bit else mine)
        bit *= 2
    return other


def nearest(me, step, n):
    bound = n * n
    found = 0
    for at in range(n):
        by_distance = sorted(range(n), key=lambda other: (abs(other - at), other))
        apart = (me - at) * (me - at)
        found = found + by_distance[step] * (1 - lax.div(apart + (bound - 1), bound))
    return found


def kernel(
    n_ep,
    n_tp,
    tok_hbm,
    rout_hbm,
    gw_hbm,
    gain_hbm,
    wg_hbm,
    wu_hbm,
    wd_hbm,
    out_ref,
    tok_ref,
    rout_ref,
    gw_ref,
    gain_ref,
    wgu,
    wd,
    outgoing,
    rows,
    combine,
    acc_gate,
    acc_up,
    part,
    part_in,
    ret_out,
    ret_in,
    in_sem,
    gu_sem,
    down_sem,
    row_send,
    disp_recv,
    gath_send,
    gath_recv,
    part_send,
    part_recv,
    ret_recv,
    turn,
):
    ep, tp = lax.axis_index("ep"), lax.axis_index("tp")
    n_exp, width, ff = wg_hbm.shape
    n_tok, cols = tok_ref.shape
    top = rout_ref.shape[0]
    slots = n_ep * n_exp * CAP
    pair = 2 if n_ep % 2 == 0 else 1
    n_chip = n_ep // pair
    chip, core = lax.div(ep, pair), lax.rem(ep, pair)
    chips = [chip] + [nearest(chip, step, n_chip) for step in range(1, n_chip)]
    cores = [lax.rem(core + turn, pair) for turn in range(pair)]
    peers = [chips[0] * pair + k for k in cores[1:]]
    peers += [other * pair + k for other in chips[1:] for k in cores]
    hops = list(range(1, n_tp))

    small = [
        pltpu.make_async_copy(src, dst, in_sem.at[i])
        for i, (src, dst) in enumerate(
            ((rout_hbm, rout_ref), (gw_hbm, gw_ref), (tok_hbm, tok_ref), (gain_hbm, gain_ref))
        )
    ]
    for copy in small:
        copy.start()

    barrier = pltpu.get_barrier_semaphore()
    for peer in peers[::-1]:
        pl.semaphore_signal(barrier, inc=1, device_id=(peer, tp), device_id_type=MESH)
    for hop in hops[::-1]:
        pl.semaphore_signal(
            barrier, inc=1, device_id=(ep, partner(tp, hop, n_tp)), device_id_type=MESH
        )

    loads = []
    for e in range(n_exp):
        loads.append(pltpu.make_async_copy(wg_hbm.at[e], wgu.at[0, e], gu_sem))
        loads.append(pltpu.make_async_copy(wu_hbm.at[e], wgu.at[1, e], gu_sem))
    for load in loads:
        load.start()
    down_load = pltpu.make_async_copy(wd_hbm, wd, down_sem)
    down_load.start()

    slot = lax.broadcasted_iota(jnp.int32, (slots, n_tok), 0)
    group, slot_rank = slot // CAP, slot % CAP
    slot_exp = (group % n_ep) * n_exp + group // n_ep
    named = jnp.zeros((slots, n_tok), jnp.float32)
    weight = jnp.zeros((slots, n_tok), jnp.float32)
    earlier = jnp.where(
        lax.broadcasted_iota(jnp.int32, (n_tok, n_tok), 0)
        < lax.broadcasted_iota(jnp.int32, (n_tok, n_tok), 1),
        1.0,
        0.0,
    ).astype(jnp.bfloat16)
    small[0].wait()
    small[1].wait()
    for k in range(top):
        hit = rout_ref[k : k + 1, :] == slot_exp
        named = named + jnp.where(hit, 1.0, 0.0)
        weight = weight + jnp.where(hit, gw_ref[k : k + 1, :], 0.0)
    rank = jnp.dot(named.astype(jnp.bfloat16), earlier, preferred_element_type=jnp.float32)
    placing = jnp.where(rank == slot_rank.astype(jnp.float32), named, 0.0)
    small[2].wait()
    sent = jnp.dot(
        placing.astype(jnp.bfloat16), tok_ref[...], preferred_element_type=jnp.float32
    )
    outgoing[...] = sent.astype(jnp.bfloat16).reshape(n_exp, n_ep, CAP, cols)
    for e in range(n_exp):
        rows[tp, e, ep] = outgoing[e, ep]

    pl.semaphore_wait(barrier, n_ep - 1 + n_tp - 1)

    def dispatch(peer, e):
        return pltpu.make_async_remote_copy(
            src_ref=outgoing.at[e, peer],
            dst_ref=rows.at[tp, e, ep],
            send_sem=row_send,
            recv_sem=disp_recv.at[e, chip],
            device_id=(peer, tp),
            device_id_type=MESH,
        )

    def gather(src, hop, e, s, count):
        return pltpu.make_async_remote_copy(
            src_ref=src,
            dst_ref=rows.at[tp, e, pl.ds(s, count)],
            send_sem=gath_send,
            recv_sem=gath_recv.at[e, hop - 1],
            device_id=(ep, partner(tp, hop, n_tp)),
            device_id_type=MESH,
        )

    def reduce(hop, e, c):
        q = partner(tp, hop, n_tp)
        return pltpu.make_async_remote_copy(
            src_ref=part.at[q, e, pl.ds(c * pair, pair)],
            dst_ref=part_in.at[e, c, hop - 1],
            send_sem=part_send,
            recv_sem=part_recv.at[e, c],
            device_id=(ep, q),
            device_id_type=MESH,
        )

    def give_back(peer, e):
        return pltpu.make_async_remote_copy(
            src_ref=ret_out.at[e, peer],
            dst_ref=ret_in.at[e, ep],
            send_sem=row_send,
            recv_sem=ret_recv,
            device_id=(peer, tp),
            device_id_type=MESH,
        )

    def landed(ref, sem):
        pltpu.make_async_copy(ref, ref, sem).wait()

    def piece(hidden, q, e):
        at = pl.multiple_of(q * cols, cols)
        part[q, e] = (
            jnp.dot(hidden, wd[e, :, pl.ds(at, cols)], preferred_element_type=jnp.float32)
            .reshape(n_ep, CAP, cols)
            .astype(jnp.bfloat16)
        )

    def finish(pre_gate, pre_up, factor, e):
        clamped = jnp.minimum(pre_gate * factor, clamp_limit)
        upper = jnp.clip(pre_up * factor, -clamp_limit, clamp_limit)
        hidden = (clamped * jax.nn.sigmoid(swish_alpha * clamped) * (upper + 1.0)).astype(
            jnp.bfloat16
        )
        if not e:
            down_load.wait()
        for hop in hops[::-1]:
            piece(hidden, partner(tp, hop, n_tp), e)
            if e < n_exp - 1:
                for c in chips[:0:-1]:
                    reduce(hop, e, c).start()
        if e == n_exp - 1:
            for c in chips[:0:-1]:
                for hop in hops[::-1]:
                    reduce(hop, e, c).start()
        piece(hidden, tp, e)

    for e in range(n_exp):
        for k in cores[1:]:
            dispatch(chip * pair + k, e).start()
        for other in chips[1:]:
            for k in range(pair):
                dispatch(other * pair + k, e).start()
    for e in range(n_exp):
        for hop in hops[::-1]:
            gather(outgoing.at[e, pl.ds(ep, 1)], hop, e, ep, 1).start()

    def take(j, e):
        wide = rows[j, e].astype(jnp.float32)
        at = pl.multiple_of(j * cols, cols)
        x = wide * gain_ref[:, pl.ds(at, cols)].reshape(1, 1, cols)
        x = x.reshape(n_ep * CAP, cols).astype(jnp.bfloat16)
        y = [
            jnp.dot(x, wgu[i, e, pl.ds(at, cols), :], preferred_element_type=jnp.float32)
            for i in range(2)
        ]
        return y, jnp.sum(wide * wide, axis=2, keepdims=True)

    def forward(turns, await_rows=True, send=True):
        for e, step in turns:
            c = chips[step]
            if step == 0:
                for s in peers[: pair - 1]:
                    landed(rows.at[tp, e, s], disp_recv.at[e, c])
                    for hop in hops[:1] + hops[:0:-1]:
                        gather(rows.at[tp, e, pl.ds(s, 1)], hop, e, s, 1).start()
            else:
                here = rows.at[tp, e, pl.ds(c * pair, pair)]
                if await_rows:
                    landed(here, disp_recv.at[e, c])
                if send:
                    for hop in hops[:1] + hops[:0:-1]:
                        gather(here, hop, e, c * pair, pair).start()

    soon = [(e, 0) for e in range(n_exp)] + [(0, step) for step in range(1, n_chip)]
    later = [(e, step) for e in range(1, n_exp) for step in range(1, n_chip)]
    forward(soon)
    if pair == 2:
        pl.when(core == 0)(lambda: forward(later))
        pl.when(core != 0)(lambda: forward(later, send=False))
    else:
        forward(later)
    squares = []
    small[3].wait()
    landed(wgu, gu_sem)
    for e in range(n_exp):
        (acc_gate[e], acc_up[e]), ssq = take(tp, e)
        squares.append(ssq)
    if pair == 2:

        @pl.when(core == 0)
        def _():
            pl.semaphore_signal(turn, inc=1, device_id=(ep + 1, tp), device_id_type=MESH)

        @pl.when(core != 0)
        def _():
            pl.semaphore_wait(turn, 1)
            forward(later, await_rows=False)

    combine[...] = (placing * weight).T

    for e in range(n_exp):
        ssq = squares[e]
        gate, up = acc_gate[e], acc_up[e]
        for hop in hops:
            j = partner(tp, hop, n_tp)
            landed(rows.at[j, e], gath_recv.at[e, (hop if n_tp & (n_tp - 1) == 0 else n_tp - hop) - 1])
            (more_gate, more_up), more = take(j, e)
            gate, up, ssq = gate + more_gate, up + more_up, ssq + more
        factor = lax.rsqrt(ssq / width + norm_eps).reshape(n_ep * CAP, 1)
        finish(gate, up, factor, e)
    for e in range(n_exp):
        for hop in hops[::-1]:
            reduce(hop, e, chip).start()

    turns = [(e, step) for e in range(n_exp) for step in range(n_chip - 1, 0, -1)]
    turns += [(e, 0) for e in range(n_exp)]
    for e, step in turns:
        c = chips[step]
        landed(part_in.at[e, c], part_recv.at[e, c])
        total = part[tp, e, pl.ds(c * pair, pair)].astype(jnp.float32)
        for hop in hops:
            total = total + part_in[e, c, hop - 1].astype(jnp.float32)
        ret_out[e, pl.ds(c * pair, pair)] = total.astype(jnp.bfloat16)
        group = peers[step * pair - 1 : (step + 1) * pair - 1] if step else peers[: pair - 1]
        for peer in group:
            give_back(peer, e).start()
        if not step:
            ret_in[e, ep] = ret_out[e, ep]

    both = combine[...]
    high = both.astype(jnp.bfloat16)
    low = (both - high.astype(jnp.float32)).astype(jnp.bfloat16)

    others = pl.ds(0, n_ep - 1)
    landed(rows.at[pl.ds(0, n_tp - 1)], gath_send)
    landed(part.at[pl.ds(0, n_tp - 1)], part_send)
    landed(ret_in.at[:, others], ret_recv)
    back = ret_in[...].reshape(slots, cols)
    out_ref[...] = (
        jnp.dot(high, back, preferred_element_type=jnp.float32)
        + jnp.dot(low, back, preferred_element_type=jnp.float32)
    ).astype(jnp.bfloat16)
    landed(rows.at[pl.ds(0, 2), :, others], row_send)


def per_device(tokens, routing, gate_weights, norm_gain, w_gate, w_up, w_down):
    n_ep, n_tp = lax.axis_size("ep"), lax.axis_size("tp")
    n_exp, width, ff = w_gate.shape
    n_tok, cols = tokens.shape
    slots = n_ep * n_exp * CAP
    pair = 2 if n_ep % 2 == 0 else 1
    n_chip = n_ep // pair
    vmem = pl.BlockSpec(memory_space=pltpu.VMEM)
    hbm = pl.BlockSpec(memory_space=pltpu.HBM)
    bf16, f32 = jnp.bfloat16, jnp.float32
    dma = pltpu.SemaphoreType.DMA
    return pl.pallas_call(
        functools.partial(kernel, n_ep, n_tp),
        out_shape=pltpu.VMEM((n_tok, cols), bf16),
        in_specs=[hbm] * 7,
        out_specs=vmem,
        scratch_shapes=[
            pltpu.VMEM(tokens.shape, bf16),
            pltpu.VMEM(routing.shape[::-1], jnp.int32),
            pltpu.VMEM(gate_weights.shape[::-1], f32),
            pltpu.VMEM((1, width), f32),
            pltpu.VMEM((2, *w_gate.shape), bf16),
            pltpu.VMEM(w_down.shape, bf16),
            pltpu.VMEM((n_exp, n_ep, CAP, cols), bf16),
            pltpu.VMEM((n_tp, n_exp, n_ep, CAP, cols), bf16),
            pltpu.VMEM((n_tok, slots), f32),
            pltpu.VMEM((n_exp, n_ep * CAP, ff), f32),
            pltpu.VMEM((n_exp, n_ep * CAP, ff), f32),
            pltpu.VMEM((n_tp, n_exp, n_ep, CAP, cols), bf16),
            pltpu.VMEM((n_exp, n_chip, n_tp - 1, pair, CAP, cols), bf16),
            pltpu.VMEM((n_exp, n_ep, CAP, cols), bf16),
            pltpu.VMEM((n_exp, n_ep, CAP, cols), bf16),
            dma((4,)),
            dma,
            dma,
            dma,
            dma((n_exp, n_chip)),
            dma,
            dma((n_exp, n_tp - 1)),
            dma,
            dma((n_exp, n_chip)),
            dma,
            pltpu.SemaphoreType.REGULAR,
        ],
        compiler_params=pltpu.CompilerParams(collective_id=0, has_side_effects=True),
    )(tokens, routing.T, gate_weights.T, norm_gain.reshape(1, width), w_gate, w_up, w_down)


def solution(mesh):
    in_specs = (
        P("ep", "tp"),
        P("ep", None),
        P("ep", None),
        P(),
        P("ep", None, "tp"),
        P("ep", None, "tp"),
        P("ep", "tp", None),
    )
    return jax.shard_map(
        per_device, mesh=mesh, in_specs=in_specs, out_specs=P("ep", "tp"), check_vma=False
    )
```
